32 devices in a mesh: sp: 4 (over y, core), tp: 8 (over z, x).
Axes of the slice: x: 2, y: 2, z: 4, core: 2. Of those that a mesh axis runs over, the one named last changes fastest.
Arguments:
- latent: bfloat16 [960, 2048], P(('sp', 'tp')), may hold values from -40 to 40
- context: bfloat16 [768, 2048], P('sp'), may hold values from -6 to 6
- cond_latent: float32 [2048], P('sp'), may hold values from -6 to 6
- cond_context: float32 [2048], P('sp'), may hold values from -6 to 6
- mod_weight: bfloat16 [2048, 6144], P('sp', 'tp'), may hold values from -0.125 to 0.125
- w_query: bfloat16 [2048, 1024], P(None, 'tp'), may hold values from -5 to 5
- w_key: bfloat16 [2048, 1024], P(None, 'tp'), may hold values from -5 to 5
- w_value: bfloat16 [2048, 1024], P(None, 'tp'), may hold values from -0.125 to 0.125
- w_out: bfloat16 [1024, 2048], P('tp'), may hold values from -0.1875 to 0.1875
- head_lambda: float32 [8], P('tp'), may hold values from 0.3 to 0.8
Outputs:
- mixed_latent: bfloat16 [960, 2048], P(('sp', 'tp'))
The draws below stay inside these ranges and needn't reach their ends.
All inputs are finite; a program needn't handle non-finite values.
Results may differ from the reference program's by a relative error of at most 0.011.
Values may be sent and summed in bfloat16 or wider, within the bound.
A program may use at most 64 MiB of HBM per device.

```python
import jax
import jax.numpy as jnp
from jax import lax

D = 2048
QK_DIM = 64
VAL_DIM = 128
HEADS = 8
GRID_W = 64
CTX = 768
TOKENS = 960


def draw_w_query(key, part):
    projection = jax.random.truncated_normal(jax.random.fold_in(key, 21), -4.0, 4.0, (D, HEADS * 2 * QK_DIM), jnp.float32) * D ** (-0.5)
    return projection.astype(jnp.bfloat16)


def draw_w_key(key, part):
    projection = jax.random.truncated_normal(jax.random.fold_in(key, 22), -4.0, 4.0, (D, HEADS * 2 * QK_DIM), jnp.float32) * D ** (-0.5)
    return projection.astype(jnp.bfloat16)


def draw_latent(key, part):
    filled = jax.random.truncated_normal(jax.random.fold_in(key, 31), -4.0, 4.0, (TOKENS, D), jnp.float32)
    return filled.astype(jnp.bfloat16)


def level_of(rng, dims, shards, low, high):
    gain, own = 1.0, jax.random.fold_in(rng, 6)
    for position, blocks in shards:
        heights = jnp.exp(jax.random.uniform(jax.random.fold_in(own, position), (blocks,), jnp.float32, low / len(shards), high / len(shards)))
        gain = gain * jnp.repeat(heights, dims[position] // blocks).reshape([-1 if axis == position else 1 for axis in range(len(dims))])
    return gain


def centred(key, dims, spread, reach, shards=(), held_as=jnp.bfloat16):
    gain = level_of(key, dims, shards, -0.22, 0.18) if shards else 1.0
    values = jax.random.normal(key, dims, jnp.float32) * spread * gain
    return jnp.minimum(jnp.maximum(values, -reach), reach).astype(held_as)


def setup_inputs(seed: int = 0) -> dict:
    seeds = jax.random.split(jax.random.key(seed), 11)
    latent = draw_latent(jax.random.fold_in(seeds[10], 71), 0)
    context = centred(seeds[1], (CTX, D), 1.0, 6.0, ((0, 4),))
    cond_latent = centred(seeds[2], (D,), 1.0, 6.0, ((0, 4),), jnp.float32)
    cond_context = centred(seeds[3], (D,), 1.0, 6.0, ((0, 4),), jnp.float32)
    mod_weight = centred(seeds[4], (D, 3 * D), D ** -0.5, 0.125, ((0, 4), (1, 8)))
    w_query = draw_w_query(jax.random.fold_in(seeds[10], 71), 0)
    w_key = draw_w_key(jax.random.fold_in(seeds[10], 71), 0)
    w_value = centred(seeds[7], (D, HEADS * VAL_DIM), D ** -0.5, 0.125, ((1, 8),))
    w_out = centred(seeds[8], (HEADS * VAL_DIM, D), (HEADS * VAL_DIM) ** -0.5, 0.1875, ((0, 8),))
    head_lambda = jnp.clip(0.3 + 0.5 * jax.random.uniform(seeds[9], (HEADS,), jnp.float32) ** level_of(seeds[9], (HEADS,), ((0, 8),), -0.2, 0.2), 0.3, 0.8)
    return dict(latent=latent, context=context, cond_latent=cond_latent, cond_context=cond_context, mod_weight=mod_weight, w_query=w_query, w_key=w_key, w_value=w_value, w_out=w_out, head_lambda=head_lambda)


NORM_EPS = 0.01
HEAD_EPS = 0.001
THETA = 10000.0

def modulate_rows(rows, shift, scale):
    values = rows.astype(jnp.float32)
    normed = values * lax.rsqrt(lax.optimization_barrier(jnp.mean(values * values, axis=-1, keepdims=True)) + NORM_EPS)
    return (normed * (1.0 + scale) + shift).astype(jnp.bfloat16)

def rotary_tables(positions):
    quarter = QK_DIM // 4
    inverse = THETA ** (-jnp.arange(quarter, dtype=jnp.float32) / quarter)
    grid_row = (positions // GRID_W).astype(jnp.float32)
    grid_column = (positions % GRID_W).astype(jnp.float32)
    by_row = grid_row[:, None] * inverse[None, :]
    by_column = grid_column[:, None] * inverse[None, :]
    angle = jnp.concatenate([by_row, by_row, by_column, by_column], axis=-1)
    return (jnp.cos(angle), jnp.sin(angle))

def rotate(product, cosine, sine):
    number = product.shape[0]
    quarter = QK_DIM // 4
    half = QK_DIM // 2
    shaped = product.reshape(number, -1, QK_DIM)
    first = shaped[..., :half]
    second = shaped[..., half:]
    turned = jnp.concatenate([-first[..., quarter:], first[..., :quarter], -second[..., quarter:], second[..., :quarter]], axis=-1)
    result = shaped * cosine[:, None, :] + turned * sine[:, None, :]
    return result.reshape(number, -1).astype(jnp.bfloat16)

def one_head(inputs):
    queries, keys, values, factor = inputs
    scores = jnp.einsum('qmd,kmd->mqk', queries.astype(jnp.float32), keys.astype(jnp.float32)) * QK_DIM ** (-0.5)
    highest = lax.optimization_barrier(jnp.max(scores, axis=-1, keepdims=True))
    weights = jnp.exp(scores - highest)
    totals = lax.optimization_barrier(jnp.sum(weights, axis=-1))
    rounded = lax.optimization_barrier(weights.astype(jnp.bfloat16))
    mixed = jnp.einsum('mqk,kd->mqd', rounded.astype(jnp.float32), values.astype(jnp.float32))
    head_out = mixed[0] / totals[0][:, None] - factor * mixed[1] / totals[1][:, None]
    head_out = head_out * lax.rsqrt(lax.optimization_barrier(jnp.mean(head_out * head_out, axis=-1, keepdims=True)) + HEAD_EPS)
    return head_out.astype(jnp.bfloat16)

def reference(latent, context, cond_latent, cond_context, mod_weight, w_query, w_key, w_value, w_out, head_lambda):
    width = latent.shape[1]
    conditioned = jax.nn.silu(jnp.stack([cond_latent, cond_context]).astype(jnp.float32)).astype(jnp.bfloat16)
    modulation = jnp.dot(conditioned, mod_weight, preferred_element_type=jnp.float32)
    normed_latent = modulate_rows(latent, modulation[0, :width], modulation[0, width:2 * width])
    normed_context = modulate_rows(context, modulation[1, :width], modulation[1, width:2 * width])
    cosine, sine = rotary_tables(jnp.arange(TOKENS, dtype=jnp.int32))
    queries = rotate(jnp.dot(normed_latent, w_query, preferred_element_type=jnp.float32), cosine, sine)
    latent_keys = rotate(jnp.dot(normed_latent, w_key, preferred_element_type=jnp.float32), cosine, sine)
    latent_values = jnp.dot(normed_latent, w_value, preferred_element_type=jnp.float32).astype(jnp.bfloat16)
    context_keys = jnp.dot(normed_context, w_key, preferred_element_type=jnp.float32).astype(jnp.bfloat16)
    context_values = jnp.dot(normed_context, w_value, preferred_element_type=jnp.float32).astype(jnp.bfloat16)
    keys = jnp.concatenate([latent_keys, context_keys], axis=0)
    values = jnp.concatenate([latent_values, context_values], axis=0)
    heads = head_lambda.shape[0]
    key_count = keys.shape[0]
    query_heads = jnp.transpose(queries.reshape(TOKENS, heads, 2, QK_DIM), (1, 0, 2, 3))
    key_heads = jnp.transpose(keys.reshape(key_count, heads, 2, QK_DIM), (1, 0, 2, 3))
    value_heads = jnp.transpose(values.reshape(key_count, heads, VAL_DIM), (1, 0, 2))
    attended = lax.map(one_head, (query_heads, key_heads, value_heads, head_lambda.astype(jnp.float32)))
    attended = jnp.transpose(attended, (1, 0, 2)).reshape(TOKENS, heads * VAL_DIM)
    projected = jnp.dot(attended, w_out, preferred_element_type=jnp.float32)
    branch = projected * lax.rsqrt(lax.optimization_barrier(jnp.mean(projected * projected, axis=-1, keepdims=True)) + NORM_EPS)
    return (latent.astype(jnp.float32) + modulation[0, 2 * width:] * branch).astype(jnp.bfloat16)
```

```python
import functools

import jax
import jax.numpy as jnp
import numpy as np
from jax import lax
from jax.experimental import pallas as pl
from jax.experimental.pallas import tpu as pltpu
from jax.sharding import PartitionSpec as P

QK_DIM = 64
VAL_DIM = 128
GRID_W = 64
NORM_EPS = 0.01
HEAD_EPS = 0.001
THETA = 10000.0
F32 = jnp.float32
BF16 = jnp.bfloat16


def rotary_tables(nsp, ntp, rows, padded):
    quarter = QK_DIM // 4
    inverse = np.float32(THETA) ** (-np.arange(quarter, dtype=np.float32) / quarter)
    p = np.arange(nsp * ntp * rows)
    r = (p // GRID_W).astype(np.float32)[:, None] * inverse
    c = (p % GRID_W).astype(np.float32)[:, None] * inverse
    angle = np.concatenate([r, r, c, c] * 2, axis=-1).astype(np.float32)
    sign = np.where(np.arange(2 * QK_DIM) % (2 * quarter) < quarter, -1.0, 1.0)
    both = np.concatenate([np.cos(angle), np.sin(angle) * sign], axis=-1).astype(np.float32)
    full = np.zeros((nsp * ntp, padded, 4 * QK_DIM), np.float32)
    full[:, :rows] = both.reshape(nsp * ntp, rows, -1)
    return full.reshape(nsp, ntp * padded, -1)


def kernel(
    nsp, ntp, rows, padded, ctx, width, modcols, qb,
    latent, context, condl, condc, modw, wq, wk, wv, wout, lam, table,
    out,
    raw, ctxv, modwv, wcat, wo, tab, part, mods, nbuf, nctx, kv, qbuf, att, att2, send, outb,
    loc, rsend, rrecv, p1s, p1r, p2s, p2r, kvs, kvf, kvr, ws, wr, ats, atr, os, orr,
):
    sp, tp = lax.axis_index("sp"), lax.axis_index("tp")
    zn, yn = ntp // 2, nsp // 2
    zi, xi = tp // 2, lax.rem(tp, 2)
    yi, ci = sp // 2, lax.rem(sp, 2)
    xpeer = zi * 2 + (1 - xi)
    cpeer = yi * 2 + (1 - ci)
    latrows = ntp * padded
    block_rows = latrows + ctx

    def local(i, src, dst):
        return pltpu.make_async_copy(src, dst, loc.at[i])

    def remote(src, dst, ss, rs, to_sp, to_tp):
        return pltpu.make_async_remote_copy(
            src_ref=src, dst_ref=dst, send_sem=ss, recv_sem=rs,
            device_id=(to_sp, to_tp), device_id_type=pl.DeviceIdType.MESH,
        )

    copies = [
        local(0, latent, raw.at[tp]),
        local(1, modw, modwv),
        local(2, context, ctxv),
        local(3, wk, wcat.at[:, pl.ds(0, 128)]),
        local(4, wv, wcat.at[:, pl.ds(128, 128)]),
        local(5, wq, wcat.at[:, pl.ds(256, 128)]),
        local(6, table.at[sp], tab),
        local(7, wout, wo.at[xi]),
    ]
    for c in copies:
        c.start()

    barrier = pltpu.get_barrier_semaphore()

    @pl.loop(1, ntp)
    def _(d):
        pl.semaphore_signal(
            barrier, inc=1, device_id=(sp, lax.rem(tp + d, ntp)),
            device_id_type=pl.DeviceIdType.MESH,
        )

    @pl.loop(1, nsp)
    def _(d):
        pl.semaphore_signal(
            barrier, inc=1, device_id=(lax.rem(sp + d, nsp), tp),
            device_id_type=pl.DeviceIdType.MESH,
        )

    copies[1].wait()
    cl = jax.nn.silu(condl[...]).reshape(1, -1)
    cc = jax.nn.silu(condc[...]).reshape(1, -1)
    row = lax.broadcasted_iota(jnp.int32, (8, cl.shape[1]), 0)
    cond = jnp.where(row == 0, cl, jnp.where(row == 1, cc, 0.0)).astype(BF16)
    part[sp] = jnp.dot(cond, modwv[...], preferred_element_type=F32)
    copies[0].wait()
    pl.semaphore_wait(barrier, (ntp - 1) + (nsp - 1))

    def p1(d, src):
        return remote(part.at[src], part.at[src], p1s.at[d], p1r.at[src], lax.rem(sp + d, nsp), tp)

    @pl.loop(1, nsp)
    def _(d):
        p1(d, sp).start()

    def row_copy(way, t, to):
        return remote(raw.at[t], raw.at[t], rsend.at[way, t], rrecv.at[t], sp, to)

    def up(t):
        return row_copy(0, t, lax.rem(tp + 2, ntp))

    def down(t):
        return row_copy(1, t, lax.rem(tp + ntp - 2, ntp))

    def across(t):
        return row_copy(2, t, xpeer)

    def forward(t, from_below):
        if from_below is not False:

            @pl.when(zi < zn - 1)
            def _():
                up(t).start()

        if from_below is not True:

            @pl.when(zi > 0)
            def _():
                down(t).start()

        across(t).start()

    forward(tp, None)
    copies[7].wait()

    def row_step(s):
        @pl.when(zi - s >= 0)
        def _():
            t = tp - 2 * s
            across(t).wait_recv()
            forward(t, True)

        @pl.when(zi + s < zn)
        def _():
            t = tp + 2 * s
            across(t).wait_recv()
            forward(t, False)

    @pl.loop(1, nsp)
    def _(d):
        p1(d, lax.rem(sp + nsp - d, nsp)).wait_recv()

    total = part[0]
    for k in range(1, nsp):
        total = total + part[k]
    mods[tp] = total

    def p2(d, src):
        return remote(mods.at[src], mods.at[src], p2s.at[d], p2r.at[src], sp, lax.rem(tp + d, ntp))

    @pl.loop(1, ntp)
    def _(d):
        p2(d, tp).start()

    row_step(1)

    @pl.loop(1, ntp)
    def _(d):
        p2(d, lax.rem(tp + ntp - d, ntp)).wait_recv()

    mod = jnp.concatenate([mods[t] for t in range(ntp)], axis=1)
    shift_l, shift_c = mod[0:1, :width], mod[1:2, :width]
    scale_l, scale_c = 1.0 + mod[0:1, width : 2 * width], 1.0 + mod[1:2, width : 2 * width]
    gate = mod[0:1, 2 * width :]

    def normed(x, scale, shift):
        x = x.astype(F32)
        x = x * lax.rsqrt(jnp.mean(x * x, axis=-1, keepdims=True) + NORM_EPS)
        return (x * scale + shift).astype(BF16)

    copies[2].wait()
    nctx[...] = normed(ctxv[...], scale_c, shift_c)
    copies[3].wait()
    copies[4].wait()
    lat_part, ctx_part = pl.ds(0, latrows), pl.ds(latrows, ctx)
    kv[sp, latrows:block_rows, :] = jnp.dot(
        nctx[...], wcat[:, 0:256], preferred_element_type=F32
    ).astype(BF16)

    def kv_direct(which, d, src):
        piece = (lat_part, ctx_part)[which]
        return remote(
            kv.at[src, piece], kv.at[src, piece], kvs.at[which, d], kvr.at[which, src],
            lax.rem(sp + 2 * d, nsp), tp,
        )

    def kv_forward(which, src):
        piece = (lat_part, ctx_part)[which]
        return remote(
            kv.at[src, piece], kv.at[src, piece], kvf.at[which, src], kvr.at[which, src], cpeer, tp
        )

    def kv_send(which):
        for d in range(1, yn):
            kv_direct(which, d, sp).start()
        kv_forward(which, sp).start()

    def kv_relay(which):
        for d in range(1, yn):
            src = lax.rem(sp + nsp - 2 * d, nsp)
            kv_direct(which, d, src).wait_recv()
            kv_forward(which, src).start()

    def kv_finish(which):
        for y in range(yn):
            kv_forward(which, y * 2 + (1 - ci)).wait_recv()

    kv_send(1)
    for s in range(2, zn):
        row_step(s)
    wo_copy = remote(wo.at[xi], wo.at[xi], ws, wr.at[xi], sp, xpeer)
    wo_copy.start()
    kv_relay(1)

    nbuf[...] = jnp.zeros_like(nbuf)

    def norm_row(t):
        nbuf[t, 0:rows, :] = normed(raw[t], scale_l, shift_l)

    for z in range(zn):
        norm_row(z * 2 + xi)
    for z in range(zn):
        t = z * 2 + (1 - xi)
        across(t).wait_recv()
        norm_row(t)
    copies[5].wait()
    copies[6].wait()
    x = nbuf[...].reshape(latrows, width)
    pkv = jnp.dot(x, wcat[:, 0:256], preferred_element_type=F32)
    cosine, sine = tab[:, 0:128], tab[:, 128:256]
    quarter = QK_DIM // 4
    lane = lax.broadcasted_iota(jnp.int32, (1, 128), 1)
    low = lax.rem(lane, 2 * quarter) < quarter

    def rotate(u):
        turned = jnp.where(low, pltpu.roll(u, 128 - quarter, 1), pltpu.roll(u, quarter, 1))
        return (u * cosine + turned * sine).astype(BF16)

    kv[sp, 0:latrows, 0:128] = rotate(pkv[:, 0:128])
    kv[sp, 0:latrows, 128:256] = pkv[:, 128:256].astype(BF16)
    kv_send(0)
    q = rotate(jnp.dot(x, wcat[:, 256:384], preferred_element_type=F32)) * BF16(QK_DIM**-0.5)
    qbuf[0] = jnp.where(lane < QK_DIM, q, BF16(0))
    qbuf[1] = jnp.where(lane < QK_DIM, BF16(0), q)
    kv_relay(0)
    kv_finish(1)
    kv_finish(0)

    keys = nsp * block_rows
    col = lax.rem(lax.broadcasted_iota(jnp.int32, (1, keys), 1), block_rows)
    empty = jnp.logical_and(col < latrows, lax.rem(col, padded) >= rows)
    bias = jnp.where(empty, F32(-1e30), F32(0.0))
    factor = lam[0]

    @pl.loop(0, latrows // qb)
    def _(i):
        here = pl.ds(pl.multiple_of(i * qb, qb), qb)
        mixed = []
        for m in range(2):
            s = lax.dot_general(
                qbuf[m, here, :], kv[:, :, 0:128].reshape(keys, 128), (((1,), (1,)), ((), ())),
                preferred_element_type=F32,
            ) + bias
            w = jnp.exp(s - jnp.max(s, axis=-1, keepdims=True))
            t = jnp.sum(w, axis=-1, keepdims=True)
            o = jnp.dot(
                w.astype(BF16), kv[:, :, 128:256].reshape(keys, 128), preferred_element_type=F32
            )
            mixed.append(o / t)
        h = mixed[0] - factor * mixed[1]
        h = h * lax.rsqrt(jnp.mean(h * h, axis=-1, keepdims=True) + HEAD_EPS)
        att[here, :] = h.astype(BF16)

    for z in range(zn):
        for x01 in range(2):
            att2[x01, z] = att[(z * 2 + x01) * padded : (z * 2 + x01 + 1) * padded, :]
    at_copy = remote(att2.at[1 - xi], att2.at[2], ats, atr, sp, xpeer)
    at_copy.start()
    remote(wo.at[1 - xi], wo.at[1 - xi], ws, wr.at[1 - xi], sp, xpeer).wait_recv()
    at_copy.wait_recv()
    w_mine, w_other = wo[xi], wo[1 - xi]

    def out_copy(d, src):
        to = lax.rem(zi + d, zn) * 2 + xi
        return remote(send.at[d], outb.at[src], os.at[d], orr.at[src], sp, to)

    for d in range(zn - 1, -1, -1):
        z = lax.rem(zi + d, zn)
        y = jnp.dot(att2[xi, z], w_mine, preferred_element_type=F32) + jnp.dot(
            att2[2, z], w_other, preferred_element_type=F32
        )
        if d:
            send[d] = y.astype(BF16)
            out_copy(d, zi).start()
    branch = y
    for d in range(1, zn):
        src = lax.rem(zi + zn - d, zn)
        out_copy(d, src).wait_recv()
        branch = branch + outb[src].astype(F32)
    branch = branch * lax.rsqrt(jnp.mean(branch * branch, axis=-1, keepdims=True) + NORM_EPS)
    out[...] = (raw[tp].astype(F32) + gate * branch[:rows]).astype(BF16)

    @pl.loop(1, nsp)
    def _(d):
        p1(d, sp).wait_send()

    @pl.loop(1, ntp)
    def _(d):
        p2(d, tp).wait_send()

    for z in range(zn):
        t = z * 2 + xi

        @pl.when(jnp.logical_and(z <= zi, zi < zn - 1))
        def _():
            up(t).wait_send()

        @pl.when(jnp.logical_and(z >= zi, zi > 0))
        def _():
            down(t).wait_send()

        across(t).wait_send()
    for which in range(2):
        for d in range(1, yn):
            kv_direct(which, d, sp).wait_send()
        for y in range(yn):
            kv_forward(which, y * 2 + ci).wait_send()
    wo_copy.wait_send()
    at_copy.wait_send()
    for d in range(1, zn):
        out_copy(d, zi).wait_send()


def shards(nsp, ntp, latent, context, condl, condc, modw, wq, wk, wv, wout, lam):
    rows, width = latent.shape
    ctx = context.shape[0]
    padded = -(-rows // 16) * 16
    latrows = ntp * padded
    block_rows = latrows + ctx
    modcols = modw.shape[1]
    zn = ntp // 2
    qb = latrows
    while qb % 32 == 0 and qb * nsp * block_rows * 4 > 1_000_000:
        qb //= 2
    table = jnp.asarray(rotary_tables(nsp, ntp, rows, padded))
    anyspace = pl.BlockSpec(memory_space=pl.ANY)
    vmem = pl.BlockSpec(memory_space=pltpu.VMEM)
    smem = pl.BlockSpec(memory_space=pltpu.SMEM)
    dma = pltpu.SemaphoreType.DMA
    return pl.pallas_call(
        functools.partial(kernel, nsp, ntp, rows, padded, ctx, width, modcols, qb),
        out_shape=jax.ShapeDtypeStruct((rows, width), BF16),
        in_specs=[anyspace, anyspace, vmem, vmem] + [anyspace] * 5 + [smem, anyspace],
        out_specs=vmem,
        scratch_shapes=[
            pltpu.VMEM((ntp, rows, width), BF16),
            pltpu.VMEM((ctx, width), BF16),
            pltpu.VMEM(modw.shape, BF16),
            pltpu.VMEM((width, 384), BF16),
            pltpu.VMEM((2,) + wout.shape, BF16),
            pltpu.VMEM((latrows, 256), F32),
            pltpu.VMEM((nsp, 8, modcols), F32),
            pltpu.VMEM((ntp, 8, modcols), F32),
            pltpu.VMEM((ntp, padded, width), BF16),
            pltpu.VMEM((ctx, width), BF16),
            pltpu.VMEM((nsp, block_rows, 256), BF16),
            pltpu.VMEM((2, latrows, 128), BF16),
            pltpu.VMEM((latrows, 128), BF16),
            pltpu.VMEM((3, zn, padded, 128), BF16),
            pltpu.VMEM((zn, padded, width), BF16),
            pltpu.VMEM((zn, padded, width), BF16),
            dma((8,)), dma((3, ntp)), dma((ntp,)), dma((nsp,)), dma((nsp,)), dma((ntp,)),
            dma((ntp,)), dma((2, nsp)), dma((2, nsp)), dma((2, nsp)), dma, dma((2,)), dma, dma,
            dma((zn,)), dma((zn,)),
        ],
        compiler_params=pltpu.CompilerParams(
            collective_id=0, has_side_effects=True, vmem_limit_bytes=60 * 1024 * 1024
        ),
    )(latent, context, condl, condc, modw, wq, wk, wv, wout, lam, table)


def solution(mesh):
    nsp, ntp = mesh.shape["sp"], mesh.shape["tp"]
    placed = (
        P(("sp", "tp"), None),
        P("sp", None),
        P("sp"),
        P("sp"),
        P("sp", "tp"),
        P(None, "tp"),
        P(None, "tp"),
        P(None, "tp"),
        P("tp", None),
        P("tp"),
    )
    return jax.shard_map(
        functools.partial(shards, nsp, ntp), mesh=mesh, in_specs=placed,
        out_specs=P(("sp", "tp"), None), check_vma=False,
    )
```

```python
import functools

import jax
import jax.numpy as jnp
import numpy as np
from jax import lax
from jax.experimental import pallas as pl
from jax.experimental.pallas import tpu as pltpu
from jax.sharding import PartitionSpec as P

QK_DIM = 64
VAL_DIM = 128
GRID_W = 64
NORM_EPS = 0.01
HEAD_EPS = 0.001
THETA = 10000.0
F32 = jnp.float32
BF16 = jnp.bfloat16
NCH = 4


def rotary_tables(nsp, ntp, rows, padded):
    quarter = QK_DIM // 4
    inverse = np.float32(THETA) ** (-np.arange(quarter, dtype=np.float32) / quarter)
    p = np.arange(nsp * ntp * rows)
    r = (p // GRID_W).astype(np.float32)[:, None] * inverse
    c = (p % GRID_W).astype(np.float32)[:, None] * inverse
    angle = np.concatenate([r, r, c, c] * 2, axis=-1).astype(np.float32)
    sign = np.where(np.arange(2 * QK_DIM) % (2 * quarter) < quarter, -1.0, 1.0)
    both = np.concatenate([np.cos(angle), np.sin(angle) * sign], axis=-1).astype(np.float32)
    full = np.zeros((nsp * ntp, padded, 4 * QK_DIM), np.float32)
    full[:, :rows] = both.reshape(nsp * ntp, rows, -1)
    full = full.reshape(nsp, ntp // 2, 2, padded, -1).transpose(0, 2, 1, 3, 4)
    return np.ascontiguousarray(full).reshape(nsp, 2, ntp // 2 * padded, -1)


def kernel(
    nsp, ntp, rows, padded, ctx, width, modcols, qb,
    latent, context, condl, condc, modw, wq, wk, wv, wout, lam, table,
    out,
    raw, ctxv, modwv, wcat, wo, tab, part, mods, nbuf, nctx, kv, qbuf, att, attx, send, outb,
    loc, rsend, rrecv, p1s, p1r, p2s, p2r, kvs, kvf, kvr, ws, wr, ats, atr, os, orr,
):
    sp, tp = lax.axis_index("sp"), lax.axis_index("tp")
    zn, yn = ntp // 2, nsp // 2
    zi, xi = tp // 2, lax.rem(tp, 2)
    yi, ci = sp // 2, lax.rem(sp, 2)
    xpeer = zi * 2 + (1 - xi)
    cpeer = yi * 2 + (1 - ci)
    latrows = ntp * padded
    half = zn * padded
    block_rows = latrows + ctx
    chunk = width // NCH

    def local(i, src, dst):
        return pltpu.make_async_copy(src, dst, loc.at[i])

    def remote(src, dst, ss, rs, to_sp, to_tp):
        return pltpu.make_async_remote_copy(
            src_ref=src, dst_ref=dst, send_sem=ss, recv_sem=rs,
            device_id=(to_sp, to_tp), device_id_type=pl.DeviceIdType.MESH,
        )

    copies = [
        local(0, latent, raw.at[tp]),
        local(1, modw, modwv),
        local(2, context, ctxv),
        local(3, wk, wcat.at[:, pl.ds(0, 128)]),
        local(4, wv, wcat.at[:, pl.ds(128, 128)]),
        local(5, wq, wcat.at[:, pl.ds(256, 128)]),
        local(6, table.at[sp, xi], tab.at[0]),
        local(7, wout, wo.at[xi]),
        local(8, table.at[sp, 1 - xi], tab.at[1]),
    ]
    for c in copies:
        c.start()

    barrier = pltpu.get_barrier_semaphore()

    @pl.loop(1, ntp)
    def _(d):
        pl.semaphore_signal(
            barrier, inc=1, device_id=(sp, lax.rem(tp + d, ntp)),
            device_id_type=pl.DeviceIdType.MESH,
        )

    @pl.loop(1, nsp)
    def _(d):
        pl.semaphore_signal(
            barrier, inc=1, device_id=(lax.rem(sp + d, nsp), tp),
            device_id_type=pl.DeviceIdType.MESH,
        )

    copies[0].wait()
    pl.semaphore_wait(barrier, (ntp - 1) + (nsp - 1))

    def row_copy(way, t, c, to):
        cols = pl.ds(c * chunk, chunk)
        return remote(
            raw.at[t, :, cols], raw.at[t, :, cols], rsend.at[way, t, c], rrecv.at[t, c], sp, to
        )

    def up(t, c):
        return row_copy(0, t, c, lax.rem(tp + 2, ntp))

    def down(t, c):
        return row_copy(1, t, c, lax.rem(tp + ntp - 2, ntp))

    def across(t, c):
        return row_copy(2, t, c, xpeer)

    def forward(t, c, from_below):
        if from_below is not False:

            @pl.when(zi < zn - 1)
            def _():
                up(t, c).start()

        if from_below is not True:

            @pl.when(zi > 0)
            def _():
                down(t, c).start()

        across(t, c).start()

    for c in range(NCH):
        forward(tp, c, None)

    def row_step(s):
        for c in range(NCH):

            @pl.when(zi - s >= 0)
            def _():
                t = tp - 2 * s
                across(t, c).wait_recv()
                forward(t, c, True)

            @pl.when(zi + s < zn)
            def _():
                t = tp + 2 * s
                across(t, c).wait_recv()
                forward(t, c, False)

    copies[1].wait()
    cl = jax.nn.silu(condl[...]).reshape(1, -1)
    cc = jax.nn.silu(condc[...]).reshape(1, -1)
    row = lax.broadcasted_iota(jnp.int32, (8, cl.shape[1]), 0)
    cond = jnp.where(row == 0, cl, jnp.where(row == 1, cc, 0.0)).astype(BF16)
    part[sp] = jnp.dot(cond, modwv[...], preferred_element_type=F32)
    def p1(d, src):
        return remote(part.at[src], part.at[src], p1s.at[d], p1r.at[src], lax.rem(sp + d, nsp), tp)

    @pl.loop(1, nsp)
    def _(d):
        p1(d, sp).start()

    @pl.loop(1, nsp)
    def _(d):
        p1(d, lax.rem(sp + nsp - d, nsp)).wait_recv()

    total = part[0]
    for k in range(1, nsp):
        total = total + part[k]
    mods[tp] = total

    def p2(d, src):
        return remote(mods.at[src], mods.at[src], p2s.at[d], p2r.at[src], sp, lax.rem(tp + d, ntp))

    @pl.loop(1, ntp)
    def _(d):
        p2(d, tp).start()

    row_step(1)
    if zn > 2:
        row_step(2)

    @pl.loop(1, ntp)
    def _(d):
        p2(d, lax.rem(tp + ntp - d, ntp)).wait_recv()

    mod = jnp.concatenate([mods[t] for t in range(ntp)], axis=1)
    shift_l, shift_c = mod[0:1, :width], mod[1:2, :width]
    scale_l, scale_c = 1.0 + mod[0:1, width : 2 * width], 1.0 + mod[1:2, width : 2 * width]
    gate = mod[0:1, 2 * width :]

    def normed(x, scale, shift):
        x = x.astype(F32)
        x = x * lax.rsqrt(jnp.mean(x * x, axis=-1, keepdims=True) + NORM_EPS)
        return (x * scale + shift).astype(BF16)

    copies[2].wait()
    nctx[...] = normed(ctxv[...], scale_c, shift_c)
    copies[3].wait()
    copies[4].wait()
    pieces = (pl.ds(0, half), pl.ds(half, half), pl.ds(latrows, ctx))
    kv[sp, latrows:block_rows, :] = jnp.dot(
        nctx[...], wcat[:, 0:256], preferred_element_type=F32
    ).astype(BF16)

    def kv_direct(which, d, src):
        piece = pieces[which]
        return remote(
            kv.at[src, piece], kv.at[src, piece], kvs.at[which, d], kvr.at[which, src],
            lax.rem(sp + 2 * d, nsp), tp,
        )

    def kv_forward(which, src):
        piece = pieces[which]
        return remote(
            kv.at[src, piece], kv.at[src, piece], kvf.at[which, src], kvr.at[which, src], cpeer, tp
        )

    def kv_send(which):
        for d in range(1, yn):
            kv_direct(which, d, sp).start()
        kv_forward(which, sp).start()

    def kv_relay(which):
        for d in range(1, yn):
            src = lax.rem(sp + nsp - 2 * d, nsp)
            kv_direct(which, d, src).wait_recv()
            kv_forward(which, src).start()

    def kv_finish(which):
        for y in range(yn):
            kv_forward(which, y * 2 + (1 - ci)).wait_recv()

    kv_send(2)
    for s in range(3, zn):
        row_step(s)
    copies[7].wait()
    wo_copy = remote(wo.at[xi], wo.at[xi], ws, wr.at[xi], sp, xpeer)
    wo_copy.start()
    nbuf[...] = jnp.zeros_like(nbuf)

    quarter = QK_DIM // 4
    lane = lax.broadcasted_iota(jnp.int32, (1, 128), 1)
    low = lax.rem(lane, 2 * quarter) < quarter

    def rotate(u, k):
        turned = jnp.where(low, pltpu.roll(u, 128 - quarter, 1), pltpu.roll(u, quarter, 1))
        return (u * tab[k, :, 0:128] + turned * tab[k, :, 128:256]).astype(BF16)

    def project(k):
        x = nbuf[k * zn : (k + 1) * zn].reshape(half, width)
        pkv = jnp.dot(x, wcat[:, 0:256], preferred_element_type=F32)
        here = slice(k * half, (k + 1) * half)
        kv[sp, here, 0:128] = rotate(pkv[:, 0:128], k)
        kv[sp, here, 128:256] = pkv[:, 128:256].astype(BF16)
        kv_send(k)
        q = jnp.dot(x, wcat[:, 256:384], preferred_element_type=F32)
        q = rotate(q, k) * BF16(QK_DIM**-0.5)
        qbuf[0, here, :] = jnp.where(lane < QK_DIM, q, BF16(0))
        qbuf[1, here, :] = jnp.where(lane < QK_DIM, BF16(0), q)

    for z in range(zn):
        nbuf[z, 0:rows, :] = normed(raw[z * 2 + xi], scale_l, shift_l)
    copies[5].wait()
    copies[6].wait()
    copies[8].wait()
    project(0)
    kv_relay(2)
    for z in range(zn):
        t = z * 2 + (1 - xi)
        for c in range(NCH):
            across(t, c).wait_recv()
        nbuf[zn + z, 0:rows, :] = normed(raw[t], scale_l, shift_l)
    kv_relay(0)
    project(1)
    kv_relay(1)
    kv_finish(2)
    kv_finish(0)
    kv_finish(1)

    keys = nsp * block_rows
    col = lax.rem(lax.broadcasted_iota(jnp.int32, (1, keys), 1), block_rows)
    empty = jnp.logical_and(col < latrows, lax.rem(col, padded) >= rows)
    bias = jnp.where(empty, F32(-1e30), F32(0.0))
    factor = lam[0]

    def attend(i):
        here = pl.ds(pl.multiple_of(i * qb, qb), qb)
        mixed = []
        for m in range(2):
            s = lax.dot_general(
                qbuf[m, here, :], kv[:, :, 0:128].reshape(keys, 128), (((1,), (1,)), ((), ())),
                preferred_element_type=F32,
            ) + bias
            w = jnp.exp(s - jnp.max(s, axis=-1, keepdims=True))
            t = jnp.sum(w, axis=-1, keepdims=True)
            o = jnp.dot(
                w.astype(BF16), kv[:, :, 128:256].reshape(keys, 128), preferred_element_type=F32
            )
            mixed.append(o / t)
        h = mixed[0] - factor * mixed[1]
        h = h * lax.rsqrt(jnp.mean(h * h, axis=-1, keepdims=True) + HEAD_EPS)
        att[here, :] = h.astype(BF16)

    pl.loop(half // qb, latrows // qb)(attend)
    at_copy = remote(att.at[pl.ds(half, half)], attx, ats, atr, sp, xpeer)
    at_copy.start()
    pl.loop(0, half // qb)(attend)
    remote(wo.at[1 - xi], wo.at[1 - xi], ws, wr.at[1 - xi], sp, xpeer).wait_recv()
    at_copy.wait_recv()
    w_mine, w_other = wo[xi], wo[1 - xi]

    def out_copy(d, src):
        to = lax.rem(zi + d, zn) * 2 + xi
        return remote(send.at[d], outb.at[src], os.at[d], orr.at[src], sp, to)

    for d in range(zn - 1, -1, -1):
        z = lax.rem(zi + d, zn)
        here = pl.ds(pl.multiple_of(z * padded, padded), padded)
        y = jnp.dot(att[here, :], w_mine, preferred_element_type=F32) + jnp.dot(
            attx[here, :], w_other, preferred_element_type=F32
        )
        if d:
            send[d] = y.astype(BF16)
            out_copy(d, zi).start()
    branch = y
    for d in range(1, zn):
        src = lax.rem(zi + zn - d, zn)
        out_copy(d, src).wait_recv()
        branch = branch + outb[src].astype(F32)
    branch = branch * lax.rsqrt(jnp.mean(branch * branch, axis=-1, keepdims=True) + NORM_EPS)
    out[...] = (raw[tp].astype(F32) + gate * branch[:rows]).astype(BF16)

    @pl.loop(1, nsp)
    def _(d):
        p1(d, sp).wait_send()

    @pl.loop(1, ntp)
    def _(d):
        p2(d, tp).wait_send()

    for z in range(zn):
        for c in range(NCH):
            t = z * 2 + xi

            @pl.when(jnp.logical_and(z <= zi, zi < zn - 1))
            def _():
                up(t, c).wait_send()

            @pl.when(jnp.logical_and(z >= zi, zi > 0))
            def _():
                down(t, c).wait_send()

            across(t, c).wait_send()
    for which in range(3):
        for d in range(1, yn):
            kv_direct(which, d, sp).wait_send()
        for y in range(yn):
            kv_forward(which, y * 2 + ci).wait_send()
    wo_copy.wait_send()
    at_copy.wait_send()
    for d in range(1, zn):
        out_copy(d, zi).wait_send()


def shards(nsp, ntp, latent, context, condl, condc, modw, wq, wk, wv, wout, lam):
    rows, width = latent.shape
    ctx = context.shape[0]
    padded = -(-rows // 16) * 16
    latrows = ntp * padded
    block_rows = latrows + ctx
    modcols = modw.shape[1]
    zn = ntp // 2
    qb = latrows // 2
    while qb % 32 == 0 and qb * nsp * block_rows * 4 > 1_000_000:
        qb //= 2
    table = jnp.asarray(rotary_tables(nsp, ntp, rows, padded))
    anyspace = pl.BlockSpec(memory_space=pl.ANY)
    vmem = pl.BlockSpec(memory_space=pltpu.VMEM)
    smem = pl.BlockSpec(memory_space=pltpu.SMEM)
    dma = pltpu.SemaphoreType.DMA
    return pl.pallas_call(
        functools.partial(kernel, nsp, ntp, rows, padded, ctx, width, modcols, qb),
        out_shape=jax.ShapeDtypeStruct((rows, width), BF16),
        in_specs=[anyspace, anyspace, vmem, vmem] + [anyspace] * 5 + [smem, anyspace],
        out_specs=vmem,
        scratch_shapes=[
            pltpu.VMEM((ntp, rows, width), BF16),
            pltpu.VMEM((ctx, width), BF16),
            pltpu.VMEM(modw.shape, BF16),
            pltpu.VMEM((width, 384), BF16),
            pltpu.VMEM((2,) + wout.shape, BF16),
            pltpu.VMEM((2, latrows // 2, 256), F32),
            pltpu.VMEM((nsp, 8, modcols), F32),
            pltpu.VMEM((ntp, 8, modcols), F32),
            pltpu.VMEM((ntp, padded, width), BF16),
            pltpu.VMEM((ctx, width), BF16),
            pltpu.VMEM((nsp, block_rows, 256), BF16),
            pltpu.VMEM((2, latrows, 128), BF16),
            pltpu.VMEM((latrows, 128), BF16),
            pltpu.VMEM((latrows // 2, 128), BF16),
            pltpu.VMEM((zn, padded, width), BF16),
            pltpu.VMEM((zn, padded, width), BF16),
            dma((9,)), dma((3, ntp, NCH)), dma((ntp, NCH)), dma((nsp,)), dma((nsp,)), dma((ntp,)),
            dma((ntp,)), dma((3, nsp)), dma((3, nsp)), dma((3, nsp)), dma, dma((2,)), dma, dma,
            dma((zn,)), dma((zn,)),
        ],
        compiler_params=pltpu.CompilerParams(
            collective_id=0, has_side_effects=True, vmem_limit_bytes=60 * 1024 * 1024
        ),
    )(latent, context, condl, condc, modw, wq, wk, wv, wout, lam, table)


def solution(mesh):
    nsp, ntp = mesh.shape["sp"], mesh.shape["tp"]
    placed = (
        P(("sp", "tp"), None),
        P("sp", None),
        P("sp"),
        P("sp"),
        P("sp", "tp"),
        P(None, "tp"),
        P(None, "tp"),
        P(None, "tp"),
        P("tp", None),
        P("tp"),
    )
    return jax.shard_map(
        functools.partial(shards, nsp, ntp), mesh=mesh, in_specs=placed,
        out_specs=P(("sp", "tp"), None), check_vma=False,
    )
```

```python
import functools

import jax
import jax.numpy as jnp
import numpy as np
from jax import lax
from jax.experimental import pallas as pl
from jax.experimental.pallas import tpu as pltpu
from jax.sharding import PartitionSpec as P

QK_DIM = 64
VAL_DIM = 128
GRID_W = 64
NORM_EPS = 0.01
HEAD_EPS = 0.001
THETA = 10000.0
F32 = jnp.float32
BF16 = jnp.bfloat16
NCH = 4


def rotary_tables(nsp, ntp, rows, padded):
    quarter = QK_DIM // 4
    inverse = np.float32(THETA) ** (-np.arange(quarter, dtype=np.float32) / quarter)
    p = np.arange(nsp * ntp * rows)
    r = (p // GRID_W).astype(np.float32)[:, None] * inverse
    c = (p % GRID_W).astype(np.float32)[:, None] * inverse
    angle = np.concatenate([r, r, c, c] * 2, axis=-1).astype(np.float32)
    sign = np.where(np.arange(2 * QK_DIM) % (2 * quarter) < quarter, -1.0, 1.0)
    both = np.concatenate([np.cos(angle), np.sin(angle) * sign], axis=-1).astype(np.float32)
    full = np.zeros((nsp * ntp, padded, 4 * QK_DIM), np.float32)
    full[:, :rows] = both.reshape(nsp * ntp, rows, -1)
    full = full.reshape(nsp, ntp // 4, 2, 2, padded, -1).transpose(0, 3, 2, 1, 4, 5)
    return np.ascontiguousarray(full).reshape(nsp, 2, 2, ntp // 4 * padded, -1)


def kernel(
    nsp, ntp, rows, padded, ctx, width, modcols, qb,
    latent, context, condl, condc, modw, wq, wk, wv, wout, lam, table,
    out,
    raw, ctxv, modwv, wcat, wo, tab, part, mods, nbuf, nctx, kv, qbuf, att, attx, send, outb,
    loc, rsend, rrecv, p1s, p1r, p2s, p2r, kvs, kvf, kvr, ws, wr, ats, atr, os, orr,
):
    sp, tp = lax.axis_index("sp"), lax.axis_index("tp")
    zn, yn = ntp // 2, nsp // 2
    zi, xi = tp // 2, lax.rem(tp, 2)
    yi, ci = sp // 2, lax.rem(sp, 2)
    xpeer = zi * 2 + (1 - xi)
    cpeer = yi * 2 + (1 - ci)
    latrows = ntp * padded
    half = zn * padded
    nq = zn // 2
    quart = nq * padded
    ki, pz = zi // 2, lax.rem(zi, 2)
    zpeer = (ki * 2 + 1 - pz) * 2 + xi
    xzpeer = (ki * 2 + 1 - pz) * 2 + 1 - xi
    block_rows = latrows + ctx
    chunk = width // NCH
    hw = wo.shape[1] // 2

    def local(i, src, dst):
        return pltpu.make_async_copy(src, dst, loc.at[i])

    def remote(src, dst, ss, rs, to_sp, to_tp):
        return pltpu.make_async_remote_copy(
            src_ref=src, dst_ref=dst, send_sem=ss, recv_sem=rs,
            device_id=(to_sp, to_tp), device_id_type=pl.DeviceIdType.MESH,
        )

    copies = [
        local(0, latent, raw.at[tp]),
        local(1, modw, modwv),
        local(2, context, ctxv),
        local(3, wk, wcat.at[:, pl.ds(0, 128)]),
        local(4, wv, wcat.at[:, pl.ds(128, 128)]),
        local(5, wq, wcat.at[:, pl.ds(256, 128)]),
        local(6, table.at[sp, xi, pz], tab.at[0, pl.ds(0, quart)]),
        local(7, wout, wo.at[0]),
        local(8, table.at[sp, 1 - xi, pz], tab.at[1, pl.ds(0, quart)]),
        local(9, table.at[sp, xi, 1 - pz], tab.at[0, pl.ds(quart, quart)]),
        local(10, table.at[sp, 1 - xi, 1 - pz], tab.at[1, pl.ds(quart, quart)]),
    ]
    for c in copies:
        c.start()

    barrier = pltpu.get_barrier_semaphore()

    @pl.loop(1, ntp)
    def _(d):
        pl.semaphore_signal(
            barrier, inc=1, device_id=(sp, lax.rem(tp + d, ntp)),
            device_id_type=pl.DeviceIdType.MESH,
        )

    @pl.loop(1, nsp)
    def _(d):
        pl.semaphore_signal(
            barrier, inc=1, device_id=(lax.rem(sp + d, nsp), tp),
            device_id_type=pl.DeviceIdType.MESH,
        )

    copies[0].wait()
    pl.semaphore_wait(barrier, (ntp - 1) + (nsp - 1))

    def row_copy(way, t, c, to):
        cols = pl.ds(c * chunk, chunk)
        return remote(
            raw.at[t, :, cols], raw.at[t, :, cols], rsend.at[way, t, c], rrecv.at[t, c], sp, to
        )

    def up(t, c):
        return row_copy(0, t, c, lax.rem(tp + 2, ntp))

    def down(t, c):
        return row_copy(1, t, c, lax.rem(tp + ntp - 2, ntp))

    def across(t, c):
        return row_copy(2, t, c, xpeer)

    def forward(t, c, from_below):
        if from_below is not False:

            @pl.when(zi < zn - 1)
            def _():
                up(t, c).start()

        if from_below is not True:

            @pl.when(zi > 0)
            def _():
                down(t, c).start()

        across(t, c).start()

    for c in range(NCH):
        forward(tp, c, None)

    def row_step(s):
        for c in range(NCH):

            @pl.when(zi - s >= 0)
            def _():
                t = tp - 2 * s
                across(t, c).wait_recv()
                forward(t, c, True)

            @pl.when(zi + s < zn)
            def _():
                t = tp + 2 * s
                across(t, c).wait_recv()
                forward(t, c, False)

    copies[1].wait()
    cl = jax.nn.silu(condl[...]).reshape(1, -1)
    cc = jax.nn.silu(condc[...]).reshape(1, -1)
    row = lax.broadcasted_iota(jnp.int32, (8, cl.shape[1]), 0)
    cond = jnp.where(row == 0, cl, jnp.where(row == 1, cc, 0.0)).astype(BF16)
    part[sp] = jnp.dot(cond, modwv[...], preferred_element_type=F32)
    def p1(d, src):
        return remote(part.at[src], part.at[src], p1s.at[d], p1r.at[src], lax.rem(sp + d, nsp), tp)

    @pl.loop(1, nsp)
    def _(d):
        p1(d, sp).start()

    @pl.loop(1, nsp)
    def _(d):
        p1(d, lax.rem(sp + nsp - d, nsp)).wait_recv()

    total = part[0]
    for k in range(1, nsp):
        total = total + part[k]
    mods[tp] = total

    def p2(d, src):
        return remote(mods.at[src], mods.at[src], p2s.at[d], p2r.at[src], sp, lax.rem(tp + d, ntp))

    @pl.loop(1, ntp)
    def _(d):
        p2(d, tp).start()

    row_step(1)
    if zn > 2:
        row_step(2)

    @pl.loop(1, ntp)
    def _(d):
        p2(d, lax.rem(tp + ntp - d, ntp)).wait_recv()

    mod = jnp.concatenate([mods[t] for t in range(ntp)], axis=1)
    shift_l, shift_c = mod[0:1, :width], mod[1:2, :width]
    scale_l, scale_c = 1.0 + mod[0:1, width : 2 * width], 1.0 + mod[1:2, width : 2 * width]
    gate = mod[0:1, 2 * width :]

    def normed(x, scale, shift):
        x = x.astype(F32)
        x = x * lax.rsqrt(jnp.mean(x * x, axis=-1, keepdims=True) + NORM_EPS)
        return (x * scale + shift).astype(BF16)

    copies[2].wait()
    nctx[...] = normed(ctxv[...], scale_c, shift_c)
    copies[3].wait()
    copies[4].wait()
    pieces = (pl.ds(0, half), pl.ds(half, half), pl.ds(latrows, ctx))
    kv[sp, latrows:block_rows, :] = jnp.dot(
        nctx[...], wcat[:, 0:256], preferred_element_type=F32
    ).astype(BF16)

    def kv_direct(which, d, src):
        piece = pieces[which]
        return remote(
            kv.at[src, piece], kv.at[src, piece], kvs.at[which, d], kvr.at[which, src],
            lax.rem(sp + 2 * d, nsp), tp,
        )

    def kv_forward(which, src):
        piece = pieces[which]
        return remote(
            kv.at[src, piece], kv.at[src, piece], kvf.at[which, src], kvr.at[which, src], cpeer, tp
        )

    def kv_send(which):
        for d in range(1, yn):
            kv_direct(which, d, sp).start()
        kv_forward(which, sp).start()

    def kv_relay(which):
        for d in range(1, yn):
            src = lax.rem(sp + nsp - 2 * d, nsp)
            kv_direct(which, d, src).wait_recv()
            kv_forward(which, src).start()

    def kv_finish(which):
        for y in range(yn):
            kv_forward(which, y * 2 + (1 - ci)).wait_recv()

    kv_send(2)
    for s in range(3, zn):
        row_step(s)
    copies[7].wait()
    mine = pl.ds(pl.multiple_of(ci * hw, hw), hw)

    def wo_copy(i, src, dst, to_sp, to_tp, core):
        return remote(wo.at[src, mine], wo.at[dst, mine], ws.at[i], wr.at[dst, core], to_sp, to_tp)

    wo_z = wo_copy(0, 0, 1, sp, zpeer, ci)
    wo_x = wo_copy(1, 0, 2, sp, xpeer, ci)
    wo_xz = wo_copy(2, 1, 3, sp, xpeer, ci)
    wo_core = [wo_copy(2 + r, r, r, cpeer, tp, ci) for r in range(1, 4)]

    def wo_arrival(r):
        other = pl.ds(pl.multiple_of((1 - ci) * hw, hw), hw)
        return remote(wo.at[r, other], wo.at[r, other], ws.at[2 + r], wr.at[r, 1 - ci], cpeer, tp)

    wo_z.start()
    wo_x.start()

    nbuf[...] = jnp.zeros_like(nbuf)

    quarter = QK_DIM // 4
    lane = lax.broadcasted_iota(jnp.int32, (1, 128), 1)
    low = lax.rem(lane, 2 * quarter) < quarter

    def rotate(u, k):
        turned = jnp.where(low, pltpu.roll(u, 128 - quarter, 1), pltpu.roll(u, quarter, 1))
        return (u * tab[k, :, 0:128] + turned * tab[k, :, 128:256]).astype(BF16)

    def project(k):
        x = nbuf[k * zn : (k + 1) * zn].reshape(half, width)
        pkv = jnp.dot(x, wcat[:, 0:256], preferred_element_type=F32)
        here = slice(k * half, (k + 1) * half)
        kv[sp, here, 0:128] = rotate(pkv[:, 0:128], k)
        kv[sp, here, 128:256] = pkv[:, 128:256].astype(BF16)
        kv_send(k)
        q = jnp.dot(x, wcat[:, 256:384], preferred_element_type=F32)
        q = rotate(q, k) * BF16(QK_DIM**-0.5)
        qbuf[0, here, :] = jnp.where(lane < QK_DIM, q, BF16(0))
        qbuf[1, here, :] = jnp.where(lane < QK_DIM, BF16(0), q)

    def position(i):
        return 2 * (i % nq) + (pz if i < nq else 1 - pz)

    for i in range(zn):
        nbuf[i, 0:rows, :] = normed(raw[position(i) * 2 + xi], scale_l, shift_l)
    copies[5].wait()
    copies[6].wait()
    for i in range(8, 11):
        copies[i].wait()
    project(0)
    kv_relay(2)
    for i in range(zn):
        t = position(i) * 2 + (1 - xi)
        for c in range(NCH):
            across(t, c).wait_recv()
        nbuf[zn + i, 0:rows, :] = normed(raw[t], scale_l, shift_l)
    kv_relay(0)
    project(1)
    wo_z.wait_recv()
    wo_xz.start()
    wo_core[0].start()
    kv_relay(1)
    kv_finish(2)
    kv_finish(0)
    kv_finish(1)

    keys = nsp * block_rows
    col = lax.rem(lax.broadcasted_iota(jnp.int32, (1, keys), 1), block_rows)
    empty = jnp.logical_and(col < latrows, lax.rem(col, padded) >= rows)
    bias = jnp.where(empty, F32(-1e30), F32(0.0))
    factor = lam[0]

    def attend(i):
        here = pl.ds(pl.multiple_of(i * qb, qb), qb)
        mixed = []
        for m in range(2):
            s = lax.dot_general(
                qbuf[m, here, :], kv[:, :, 0:128].reshape(keys, 128), (((1,), (1,)), ((), ())),
                preferred_element_type=F32,
            ) + bias
            w = jnp.exp(s - jnp.max(s, axis=-1, keepdims=True))
            t = jnp.sum(w, axis=-1, keepdims=True)
            o = jnp.dot(
                w.astype(BF16), kv[:, :, 128:256].reshape(keys, 128), preferred_element_type=F32
            )
            mixed.append(o / t)
        h = mixed[0] - factor * mixed[1]
        h = h * lax.rsqrt(jnp.mean(h * h, axis=-1, keepdims=True) + HEAD_EPS)
        att[here, :] = h.astype(BF16)

    pl.loop(half // qb, latrows // qb)(attend)
    def at_copy(r, to):
        return remote(
            att.at[pl.ds(r * quart, quart)], attx.at[:, pl.ds(r * 128, 128)],
            ats.at[r], atr.at[r], sp, to,
        )

    at = [None, at_copy(1, zpeer), at_copy(2, xpeer), at_copy(3, xzpeer)]
    at[3].start()
    at[2].start()
    wo_x.wait_recv()
    wo_core[1].start()
    pl.loop(0, half // qb)(attend)
    at[1].start()
    attx[:, 0:128] = att[0:quart, :]
    wo_xz.wait_recv()
    wo_core[2].start()
    for r in range(1, 4):
        wo_arrival(r).wait_recv()
        at[r].wait_recv()
    w_all = wo[...].reshape(4 * wo.shape[1], width)

    def out_copy(d, src):
        to = (2 * lax.rem(ki + d, nq) + pz) * 2 + xi
        return remote(send.at[d], outb.at[src], os.at[d], orr.at[src], sp, to)

    for d in range(nq - 1, -1, -1):
        here = pl.ds(pl.multiple_of(lax.rem(ki + d, nq) * padded, padded), padded)
        branch = jnp.dot(attx[here, :], w_all, preferred_element_type=F32)
        if d:
            send[d] = branch.astype(BF16)
            out_copy(d, ki).start()
    for d in range(1, nq):
        src = lax.rem(ki + nq - d, nq)
        out_copy(d, src).wait_recv()
        branch = branch + outb[src].astype(F32)
    branch = branch * lax.rsqrt(jnp.mean(branch * branch, axis=-1, keepdims=True) + NORM_EPS)
    out[...] = (raw[tp].astype(F32) + gate * branch[:rows]).astype(BF16)

    @pl.loop(1, nsp)
    def _(d):
        p1(d, sp).wait_send()

    @pl.loop(1, ntp)
    def _(d):
        p2(d, tp).wait_send()

    for z in range(zn):
        for c in range(NCH):
            t = z * 2 + xi

            @pl.when(jnp.logical_and(z <= zi, zi < zn - 1))
            def _():
                up(t, c).wait_send()

            @pl.when(jnp.logical_and(z >= zi, zi > 0))
            def _():
                down(t, c).wait_send()

            across(t, c).wait_send()
    for which in range(3):
        for d in range(1, yn):
            kv_direct(which, d, sp).wait_send()
        for y in range(yn):
            kv_forward(which, y * 2 + ci).wait_send()
    for c in [wo_z, wo_x, wo_xz] + wo_core + at[1:]:
        c.wait_send()
    for d in range(1, nq):
        out_copy(d, ki).wait_send()


def shards(nsp, ntp, latent, context, condl, condc, modw, wq, wk, wv, wout, lam):
    rows, width = latent.shape
    ctx = context.shape[0]
    padded = -(-rows // 16) * 16
    latrows = ntp * padded
    block_rows = latrows + ctx
    modcols = modw.shape[1]
    zn = ntp // 2
    qb = latrows // 2
    while qb % 32 == 0 and qb * nsp * block_rows * 4 > 1_000_000:
        qb //= 2
    table = jnp.asarray(rotary_tables(nsp, ntp, rows, padded))
    anyspace = pl.BlockSpec(memory_space=pl.ANY)
    vmem = pl.BlockSpec(memory_space=pltpu.VMEM)
    smem = pl.BlockSpec(memory_space=pltpu.SMEM)
    dma = pltpu.SemaphoreType.DMA
    return pl.pallas_call(
        functools.partial(kernel, nsp, ntp, rows, padded, ctx, width, modcols, qb),
        out_shape=jax.ShapeDtypeStruct((rows, width), BF16),
        in_specs=[anyspace, anyspace, vmem, vmem] + [anyspace] * 5 + [smem, anyspace],
        out_specs=vmem,
        scratch_shapes=[
            pltpu.VMEM((ntp, rows, width), BF16),
            pltpu.VMEM((ctx, width), BF16),
            pltpu.VMEM(modw.shape, BF16),
            pltpu.VMEM((width, 384), BF16),
            pltpu.VMEM((4,) + wout.shape, BF16),
            pltpu.VMEM((2, latrows // 2, 256), F32),
            pltpu.VMEM((nsp, 8, modcols), F32),
            pltpu.VMEM((ntp, 8, modcols), F32),
            pltpu.VMEM((ntp, padded, width), BF16),
            pltpu.VMEM((ctx, width), BF16),
            pltpu.VMEM((nsp, block_rows, 256), BF16),
            pltpu.VMEM((2, latrows, 128), BF16),
            pltpu.VMEM((latrows, 128), BF16),
            pltpu.VMEM((latrows // 4, 512), BF16),
            pltpu.VMEM((zn // 2, padded, width), BF16),
            pltpu.VMEM((zn // 2, padded, width), BF16),
            dma((11,)), dma((3, ntp, NCH)), dma((ntp, NCH)), dma((nsp,)), dma((nsp,)), dma((ntp,)),
            dma((ntp,)), dma((3, nsp)), dma((3, nsp)), dma((3, nsp)), dma((6,)), dma((4, 2)), dma((4,)), dma((4,)),
            dma((zn // 2,)), dma((zn // 2,)),
        ],
        compiler_params=pltpu.CompilerParams(
            collective_id=0, has_side_effects=True, vmem_limit_bytes=60 * 1024 * 1024
        ),
    )(latent, context, condl, condc, modw, wq, wk, wv, wout, lam, table)


def solution(mesh):
    nsp, ntp = mesh.shape["sp"], mesh.shape["tp"]
    placed = (
        P(("sp", "tp"), None),
        P("sp", None),
        P("sp"),
        P("sp"),
        P("sp", "tp"),
        P(None, "tp"),
        P(None, "tp"),
        P(None, "tp"),
        P("tp", None),
        P("tp"),
    )
    return jax.shard_map(
        functools.partial(shards, nsp, ntp), mesh=mesh, in_specs=placed,
        out_specs=P(("sp", "tp"), None), check_vma=False,
    )
```

```python
import functools

import jax
import jax.numpy as jnp
import numpy as np
from jax import lax
from jax.experimental import pallas as pl
from jax.experimental.pallas import tpu as pltpu
from jax.sharding import PartitionSpec as P

QK_DIM = 64
VAL_DIM = 128
GRID_W = 64
NORM_EPS = 0.01
HEAD_EPS = 0.001
THETA = 10000.0
F32 = jnp.float32
BF16 = jnp.bfloat16
NCH = 4


def rotary_tables(nsp, ntp, rows, padded):
    quarter = QK_DIM // 4
    inverse = np.float32(THETA) ** (-np.arange(quarter, dtype=np.float32) / quarter)
    p = np.arange(nsp * ntp * rows)
    r = (p // GRID_W).astype(np.float32)[:, None] * inverse
    c = (p % GRID_W).astype(np.float32)[:, None] * inverse
    angle = np.concatenate([r, r, c, c] * 2, axis=-1).astype(np.float32)
    sign = np.where(np.arange(2 * QK_DIM) % (2 * quarter) < quarter, -1.0, 1.0)
    both = np.concatenate([np.cos(angle), np.sin(angle) * sign], axis=-1).astype(np.float32)
    full = np.zeros((nsp * ntp, padded, 4 * QK_DIM), np.float32)
    full[:, :rows] = both.reshape(nsp * ntp, rows, -1)
    full = full.reshape(nsp, ntp // 4, 2, 2, padded, -1).transpose(0, 3, 2, 1, 4, 5)
    return np.ascontiguousarray(full).reshape(nsp, 2, 2, ntp // 4 * padded, -1)


def kernel(
    nsp, ntp, rows, padded, ctx, width, modcols, qb,
    latent, context, condl, condc, modw, wq, wk, wv, wout, lam, table,
    out,
    raw, ctxv, modwv, wcat, wo, tab, part, mods, nbuf, nctx, kv, qbuf, att, attx, send, outb,
    loc, rsend, rrecv, p1s, p1r, p2s, p2r, kvs, kvf, kvr, ws, wr, ats, atr, os, orr,
):
    sp, tp = lax.axis_index("sp"), lax.axis_index("tp")
    zn, yn = ntp // 2, nsp // 2
    zi, xi = tp // 2, lax.rem(tp, 2)
    yi, ci = sp // 2, lax.rem(sp, 2)
    xpeer = zi * 2 + (1 - xi)
    cpeer = yi * 2 + (1 - ci)
    latrows = ntp * padded
    half = zn * padded
    nq = zn // 2
    quart = nq * padded
    ki, pz = zi // 2, lax.rem(zi, 2)
    zpeer = (ki * 2 + 1 - pz) * 2 + xi
    xzpeer = (ki * 2 + 1 - pz) * 2 + 1 - xi
    block_rows = latrows + ctx
    chunk = width // NCH
    hw = wo.shape[1] // 2

    def local(i, src, dst):
        return pltpu.make_async_copy(src, dst, loc.at[i])

    def remote(src, dst, ss, rs, to_sp, to_tp):
        return pltpu.make_async_remote_copy(
            src_ref=src, dst_ref=dst, send_sem=ss, recv_sem=rs,
            device_id=(to_sp, to_tp), device_id_type=pl.DeviceIdType.MESH,
        )

    copies = [
        local(0, latent, raw.at[tp]),
        local(1, modw, modwv),
        local(2, context, ctxv),
        local(3, wk, wcat.at[:, pl.ds(0, 128)]),
        local(4, wv, wcat.at[:, pl.ds(128, 128)]),
        local(5, wq, wcat.at[:, pl.ds(256, 128)]),
        local(6, table.at[sp, xi, pz], tab.at[0, pl.ds(0, quart)]),
        local(7, wout, wo.at[0]),
        local(8, table.at[sp, 1 - xi, pz], tab.at[1, pl.ds(0, quart)]),
        local(9, table.at[sp, xi, 1 - pz], tab.at[0, pl.ds(quart, quart)]),
        local(10, table.at[sp, 1 - xi, 1 - pz], tab.at[1, pl.ds(quart, quart)]),
    ]
    for c in copies:
        c.start()

    barrier = pltpu.get_barrier_semaphore()

    @pl.loop(1, ntp)
    def _(d):
        pl.semaphore_signal(
            barrier, inc=1, device_id=(sp, lax.rem(tp + d, ntp)),
            device_id_type=pl.DeviceIdType.MESH,
        )

    @pl.loop(1, nsp)
    def _(d):
        pl.semaphore_signal(
            barrier, inc=1, device_id=(lax.rem(sp + d, nsp), tp),
            device_id_type=pl.DeviceIdType.MESH,
        )

    copies[0].wait()
    pl.semaphore_wait(barrier, (ntp - 1) + (nsp - 1))

    def row_copy(way, t, c, to):
        cols = pl.ds(c * chunk, chunk)
        return remote(
            raw.at[t, :, cols], raw.at[t, :, cols], rsend.at[way, t // 2], rrecv.at[t, c], sp, to
        )

    def up(t, c):
        return row_copy(0, t, c, lax.rem(tp + 2, ntp))

    def down(t, c):
        return row_copy(1, t, c, lax.rem(tp + ntp - 2, ntp))

    def across(t, c):
        return row_copy(2, t, c, xpeer)

    def forward(t, c, from_below):
        if from_below is not False:

            @pl.when(zi < zn - 1)
            def _():
                up(t, c).start()

        if from_below is not True:

            @pl.when(zi > 0)
            def _():
                down(t, c).start()

        across(t, c).start()

    for c in range(NCH):
        forward(tp, c, None)

    def row_step(s):
        for c in range(NCH):

            @pl.when(zi - s >= 0)
            def _():
                t = tp - 2 * s
                across(t, c).wait_recv()
                forward(t, c, True)

            @pl.when(zi + s < zn)
            def _():
                t = tp + 2 * s
                across(t, c).wait_recv()
                forward(t, c, False)

    copies[1].wait()
    cl = jax.nn.silu(condl[...]).reshape(1, -1)
    cc = jax.nn.silu(condc[...]).reshape(1, -1)
    row = lax.broadcasted_iota(jnp.int32, (8, cl.shape[1]), 0)
    cond = jnp.where(row == 0, cl, jnp.where(row == 1, cc, 0.0)).astype(BF16)
    part[sp] = jnp.dot(cond, modwv[...], preferred_element_type=F32)[0:2]
    def p1(d, src):
        return remote(part.at[src], part.at[src], p1s.at[d], p1r.at[src], lax.rem(sp + d, nsp), tp)

    @pl.loop(1, nsp)
    def _(d):
        p1(d, sp).start()

    @pl.loop(1, nsp)
    def _(d):
        p1(d, lax.rem(sp + nsp - d, nsp)).wait_recv()

    total = part[0]
    for k in range(1, nsp):
        total = total + part[k]
    mods[tp] = total

    def p2(d, src):
        return remote(mods.at[src], mods.at[src], p2s.at[d], p2r.at[src], sp, lax.rem(tp + d, ntp))

    @pl.loop(1, ntp)
    def _(d):
        p2(d, tp).start()

    row_step(1)
    if zn > 2:
        row_step(2)

    mine = pl.ds(pl.multiple_of(ci * hw, hw), hw)

    def wo_copy(i, src, dst, to_sp, to_tp, core):
        return remote(wo.at[src, mine], wo.at[dst, mine], ws.at[i], wr.at[dst, core], to_sp, to_tp)

    wo_z = wo_copy(0, 0, 1, sp, zpeer, ci)
    wo_x = wo_copy(1, 0, 2, sp, xpeer, ci)
    wo_xz = wo_copy(2, 1, 3, sp, xpeer, ci)
    wo_core = [wo_copy(2 + r, r, r, cpeer, tp, ci) for r in range(1, 4)]

    def wo_arrival(r):
        other = pl.ds(pl.multiple_of((1 - ci) * hw, hw), hw)
        return remote(wo.at[r, other], wo.at[r, other], ws.at[2 + r], wr.at[r, 1 - ci], cpeer, tp)

    copies[7].wait()
    wo_z.start()

    @pl.loop(1, ntp)
    def _(d):
        p2(d, lax.rem(tp + ntp - d, ntp)).wait_recv()

    mod = jnp.concatenate([mods[t] for t in range(ntp)], axis=1)
    shift_l, shift_c = mod[0:1, :width], mod[1:2, :width]
    scale_l, scale_c = 1.0 + mod[0:1, width : 2 * width], 1.0 + mod[1:2, width : 2 * width]
    gate = mod[0:1, 2 * width :]

    def normed(x, scale, shift):
        x = x.astype(F32)
        x = x * lax.rsqrt(jnp.mean(x * x, axis=-1, keepdims=True) + NORM_EPS)
        return (x * scale + shift).astype(BF16)

    copies[2].wait()
    nctx[...] = normed(ctxv[...], scale_c, shift_c)
    copies[3].wait()
    copies[4].wait()
    pieces = (pl.ds(0, half), pl.ds(half, half), pl.ds(latrows, ctx))
    kv[sp, latrows:block_rows, :] = jnp.dot(
        nctx[...], wcat[:, 0:256], preferred_element_type=F32
    ).astype(BF16)

    def kv_direct(which, d, src):
        piece = pieces[which]
        return remote(
            kv.at[src, piece], kv.at[src, piece], kvs.at[which, d], kvr.at[which, src],
            lax.rem(sp + 2 * d, nsp), tp,
        )

    def kv_forward(which, src):
        piece = pieces[which]
        return remote(
            kv.at[src, piece], kv.at[src, piece], kvf.at[which, src], kvr.at[which, src], cpeer, tp
        )

    def kv_send(which):
        for d in range(1, yn):
            kv_direct(which, d, sp).start()
        kv_forward(which, sp).start()

    def kv_relay(which):
        for d in range(1, yn):
            src = lax.rem(sp + nsp - 2 * d, nsp)
            kv_direct(which, d, src).wait_recv()
            kv_forward(which, src).start()

    def kv_finish(which):
        for y in range(yn):
            kv_forward(which, y * 2 + (1 - ci)).wait_recv()

    kv_send(2)
    for s in range(3, zn):
        row_step(s)
    wo_x.start()

    nbuf[...] = jnp.zeros_like(nbuf)

    quarter = QK_DIM // 4
    lane = lax.broadcasted_iota(jnp.int32, (1, 128), 1)
    low = lax.rem(lane, 2 * quarter) < quarter

    def rotate(u, k):
        turned = jnp.where(low, pltpu.roll(u, 128 - quarter, 1), pltpu.roll(u, quarter, 1))
        return (u * tab[k, :, 0:128] + turned * tab[k, :, 128:256]).astype(BF16)

    def project(k):
        x = nbuf[k * zn : (k + 1) * zn].reshape(half, width)
        pkv = jnp.dot(x, wcat[:, 0:256], preferred_element_type=F32)
        here = slice(k * half, (k + 1) * half)
        kv[sp, here, 0:128] = rotate(pkv[:, 0:128], k)
        kv[sp, here, 128:256] = pkv[:, 128:256].astype(BF16)
        kv_send(k)
        q = jnp.dot(x, wcat[:, 256:384], preferred_element_type=F32)
        q = rotate(q, k) * BF16(QK_DIM**-0.5)
        for i in range(zn):
            u = q[i * padded : (i + 1) * padded]
            d = lax.rem(i % nq + nq - ki, nq)
            to = pl.ds(pl.multiple_of((d * 4 + k * 2 + i // nq) * padded, padded), padded)
            qbuf[0, to, :] = jnp.where(lane < QK_DIM, u, BF16(0))
            qbuf[1, to, :] = jnp.where(lane < QK_DIM, BF16(0), u)

    def position(i):
        return 2 * (i % nq) + (pz if i < nq else 1 - pz)

    for i in range(zn):
        nbuf[i, 0:rows, :] = normed(raw[position(i) * 2 + xi], scale_l, shift_l)
    copies[5].wait()
    copies[6].wait()
    for i in range(8, 11):
        copies[i].wait()
    project(0)
    wo_z.wait_recv()
    wo_xz.start()
    wo_core[0].start()
    kv_relay(2)
    for i in range(zn):
        t = position(i) * 2 + (1 - xi)
        for c in range(NCH):
            across(t, c).wait_recv()
        nbuf[zn + i, 0:rows, :] = normed(raw[t], scale_l, shift_l)
    kv_relay(0)
    project(1)
    kv_relay(1)
    kv_finish(2)
    kv_finish(0)
    kv_finish(1)

    keys = nsp * block_rows
    col = lax.rem(lax.broadcasted_iota(jnp.int32, (1, keys), 1), block_rows)
    empty = jnp.logical_and(col < latrows, lax.rem(col, padded) >= rows)
    bias = jnp.where(empty, F32(-1e30), F32(0.0))
    factor = lam[0]

    def attend(i):
        here = pl.ds(pl.multiple_of(i * qb, qb), qb)
        mixed = []
        for m in range(2):
            s = lax.dot_general(
                qbuf[m, here, :], kv[:, :, 0:128].reshape(keys, 128), (((1,), (1,)), ((), ())),
                preferred_element_type=F32,
            ) + bias
            w = jnp.exp(s - jnp.max(s, axis=-1, keepdims=True))
            t = jnp.sum(w, axis=-1, keepdims=True)
            o = jnp.dot(
                w.astype(BF16), kv[:, :, 128:256].reshape(keys, 128), preferred_element_type=F32
            )
            mixed.append(o / t)
        h = mixed[0] - factor * mixed[1]
        h = h * lax.rsqrt(jnp.mean(h * h, axis=-1, keepdims=True) + HEAD_EPS)
        att[here, :] = h.astype(BF16)

    group = 4 * padded

    def at_copy(d, r, to):
        return remote(
            att.at[pl.ds(d * group + r * padded, padded)], attx.at[d, :, pl.ds(r * 128, 128)],
            ats.at[d, r], atr.at[d, r], sp, to,
        )

    def attended(d):
        pl.loop(d * (group // qb), (d + 1) * (group // qb))(attend)
        attx[d, :, 0:128] = att[d * group : d * group + padded, :]
        for r, to in ((3, xzpeer), (2, xpeer), (1, zpeer)):
            at_copy(d, r, to).start()

    attended(nq - 1)
    wo_x.wait_recv()
    wo_core[1].start()
    for d in range(nq - 2, -1, -1):
        attended(d)
    wo_xz.wait_recv()
    wo_core[2].start()
    for r in range(1, 4):
        wo_arrival(r).wait_recv()
    w_all = wo[...].reshape(4 * wo.shape[1], width)

    def out_copy(d, src):
        to = (2 * lax.rem(ki + d, nq) + pz) * 2 + xi
        return remote(send.at[d], outb.at[src], os.at[d], orr.at[src], sp, to)

    for d in range(nq - 1, -1, -1):
        for r in range(1, 4):
            at_copy(d, r, xpeer).wait_recv()
        branch = jnp.dot(attx[d], w_all, preferred_element_type=F32)
        if d:
            send[d] = branch.astype(BF16)
            out_copy(d, ki).start()
    for d in range(1, nq):
        src = lax.rem(ki + nq - d, nq)
        out_copy(d, src).wait_recv()
        branch = branch + outb[src].astype(F32)
    branch = branch * lax.rsqrt(jnp.mean(branch * branch, axis=-1, keepdims=True) + NORM_EPS)
    out[...] = (raw[tp].astype(F32) + gate * branch[:rows]).astype(BF16)

    @pl.loop(1, nsp)
    def _(d):
        p1(d, sp).wait_send()

    @pl.loop(1, ntp)
    def _(d):
        p2(d, tp).wait_send()

    for z in range(zn):

        def sent(way):
            whole = raw.at[z * 2 + xi]
            remote(whole, whole, rsend.at[way, z], rrecv.at[0, 0], sp, xpeer).wait_send()

        @pl.when(jnp.logical_and(z <= zi, zi < zn - 1))
        def _():
            sent(0)

        @pl.when(jnp.logical_and(z >= zi, zi > 0))
        def _():
            sent(1)

        sent(2)
    for which in range(3):
        for d in range(1, yn):
            kv_direct(which, d, sp).wait_send()
        for y in range(yn):
            kv_forward(which, y * 2 + ci).wait_send()
    for c in [wo_z, wo_x, wo_xz] + wo_core:
        c.wait_send()
    for d in range(nq):
        for r in range(1, 4):
            at_copy(d, r, xpeer).wait_send()
    for d in range(1, nq):
        out_copy(d, ki).wait_send()


def shards(nsp, ntp, latent, context, condl, condc, modw, wq, wk, wv, wout, lam):
    rows, width = latent.shape
    ctx = context.shape[0]
    padded = -(-rows // 16) * 16
    latrows = ntp * padded
    block_rows = latrows + ctx
    modcols = modw.shape[1]
    zn = ntp // 2
    qb = 4 * padded
    while qb % 32 == 0 and qb * nsp * block_rows * 4 > 1_000_000:
        qb //= 2
    table = jnp.asarray(rotary_tables(nsp, ntp, rows, padded))
    anyspace = pl.BlockSpec(memory_space=pl.ANY)
    vmem = pl.BlockSpec(memory_space=pltpu.VMEM)
    smem = pl.BlockSpec(memory_space=pltpu.SMEM)
    dma = pltpu.SemaphoreType.DMA
    return pl.pallas_call(
        functools.partial(kernel, nsp, ntp, rows, padded, ctx, width, modcols, qb),
        out_shape=jax.ShapeDtypeStruct((rows, width), BF16),
        in_specs=[anyspace, anyspace, vmem, vmem] + [anyspace] * 5 + [smem, anyspace],
        out_specs=vmem,
        scratch_shapes=[
            pltpu.VMEM((ntp, rows, width), BF16),
            pltpu.VMEM((ctx, width), BF16),
            pltpu.VMEM(modw.shape, BF16),
            pltpu.VMEM((width, 384), BF16),
            pltpu.VMEM((4,) + wout.shape, BF16),
            pltpu.VMEM((2, latrows // 2, 256), F32),
            pltpu.VMEM((nsp, 2, modcols), F32),
            pltpu.VMEM((ntp, 2, modcols), F32),
            pltpu.VMEM((ntp, padded, width), BF16),
            pltpu.VMEM((ctx, width), BF16),
            pltpu.VMEM((nsp, block_rows, 256), BF16),
            pltpu.VMEM((2, latrows, 128), BF16),
            pltpu.VMEM((latrows, 128), BF16),
            pltpu.VMEM((zn // 2, padded, 512), BF16),
            pltpu.VMEM((zn // 2, padded, width), BF16),
            pltpu.VMEM((zn // 2, padded, width), BF16),
            dma((11,)), dma((3, ntp // 2)), dma((ntp, NCH)), dma((nsp,)), dma((nsp,)), dma((ntp,)),
            dma((ntp,)), dma((3, nsp)), dma((3, nsp)), dma((3, nsp)), dma((6,)), dma((4, 2)), dma((zn // 2, 4)),
            dma((zn // 2, 4)),
            dma((zn // 2,)), dma((zn // 2,)),
        ],
        compiler_params=pltpu.CompilerParams(
            collective_id=0, has_side_effects=True, vmem_limit_bytes=60 * 1024 * 1024
        ),
    )(latent, context, condl, condc, modw, wq, wk, wv, wout, lam, table)


def solution(mesh):
    nsp, ntp = mesh.shape["sp"], mesh.shape["tp"]
    placed = (
        P(("sp", "tp"), None),
        P("sp", None),
        P("sp"),
        P("sp"),
        P("sp", "tp"),
        P(None, "tp"),
        P(None, "tp"),
        P(None, "tp"),
        P("tp", None),
        P("tp"),
    )
    return jax.shard_map(
        functools.partial(shards, nsp, ntp), mesh=mesh, in_specs=placed,
        out_specs=P(("sp", "tp"), None), check_vma=False,
    )
```

```python
import functools

import jax
import jax.numpy as jnp
import numpy as np
from jax import lax
from jax.experimental import pallas as pl
from jax.experimental.pallas import tpu as pltpu
from jax.sharding import PartitionSpec as P

QK_DIM = 64
VAL_DIM = 128
GRID_W = 64
NORM_EPS = 0.01
HEAD_EPS = 0.001
THETA = 10000.0
F32 = jnp.float32
BF16 = jnp.bfloat16
NCH = 4


def rotary_tables(nsp, ntp, rows, padded):
    quarter = QK_DIM // 4
    inverse = np.float32(THETA) ** (-np.arange(quarter, dtype=np.float32) / quarter)
    p = np.arange(nsp * ntp * rows)
    r = (p // GRID_W).astype(np.float32)[:, None] * inverse
    c = (p % GRID_W).astype(np.float32)[:, None] * inverse
    angle = np.concatenate([r, r, c, c] * 2, axis=-1).astype(np.float32)
    sign = np.where(np.arange(2 * QK_DIM) % (2 * quarter) < quarter, -1.0, 1.0)
    both = np.concatenate([np.cos(angle), np.sin(angle) * sign], axis=-1).astype(np.float32)
    full = np.zeros((nsp * ntp, padded, 4 * QK_DIM), np.float32)
    full[:, :rows] = both.reshape(nsp * ntp, rows, -1)
    full = full.reshape(nsp, ntp // 4, 2, 2, padded, -1).transpose(0, 3, 2, 1, 4, 5)
    return np.ascontiguousarray(full).reshape(nsp, 2, 2, ntp // 4 * padded, -1)


def kernel(
    nsp, ntp, rows, padded, ctx, width, modcols, qb,
    latent, context, condl, condc, modw, wq, wk, wv, wout, lam, table,
    out,
    raw, ctxv, modwv, wcat, wo, tab, part, mods, nbuf, nctx, kv, qbuf, att, attx, send, outb,
    loc, rsend, rrecv, p1s, p1r, p2s, p2r, kvs, kvf, kvr, ws, wr, ats, atr, os, orr,
):
    sp, tp = lax.axis_index("sp"), lax.axis_index("tp")
    zn, yn = ntp // 2, nsp // 2
    zi, xi = tp // 2, lax.rem(tp, 2)
    yi, ci = sp // 2, lax.rem(sp, 2)
    xpeer = zi * 2 + (1 - xi)
    cpeer = yi * 2 + (1 - ci)
    latrows = ntp * padded
    half = zn * padded
    nq = zn // 2
    quart = nq * padded
    ki, pz = zi // 2, lax.rem(zi, 2)
    zpeer = (ki * 2 + 1 - pz) * 2 + xi
    xzpeer = (ki * 2 + 1 - pz) * 2 + 1 - xi
    block_rows = latrows + ctx
    chunk = width // NCH
    hw = wo.shape[1] // 2

    def local(i, src, dst):
        return pltpu.make_async_copy(src, dst, loc.at[i])

    def remote(src, dst, ss, rs, to_sp, to_tp):
        return pltpu.make_async_remote_copy(
            src_ref=src, dst_ref=dst, send_sem=ss, recv_sem=rs,
            device_id=(to_sp, to_tp), device_id_type=pl.DeviceIdType.MESH,
        )

    copies = [
        local(0, latent, raw.at[tp]),
        local(1, modw, modwv),
        local(2, context, ctxv),
        local(3, wk, wcat.at[:, pl.ds(0, 128)]),
        local(4, wv, wcat.at[:, pl.ds(128, 128)]),
        local(5, wq, wcat.at[:, pl.ds(256, 128)]),
        local(6, table.at[sp, xi, pz], tab.at[0, pl.ds(0, quart)]),
        local(7, wout, wo.at[0]),
        local(8, table.at[sp, 1 - xi, pz], tab.at[1, pl.ds(0, quart)]),
        local(9, table.at[sp, xi, 1 - pz], tab.at[0, pl.ds(quart, quart)]),
        local(10, table.at[sp, 1 - xi, 1 - pz], tab.at[1, pl.ds(quart, quart)]),
    ]
    for c in copies:
        c.start()

    barrier = pltpu.get_barrier_semaphore()

    @pl.loop(1, ntp)
    def _(d):
        pl.semaphore_signal(
            barrier, inc=1, device_id=(sp, lax.rem(tp + d, ntp)),
            device_id_type=pl.DeviceIdType.MESH,
        )

    @pl.loop(1, nsp)
    def _(d):
        pl.semaphore_signal(
            barrier, inc=1, device_id=(lax.rem(sp + d, nsp), tp),
            device_id_type=pl.DeviceIdType.MESH,
        )

    copies[0].wait()
    pl.semaphore_wait(barrier, (ntp - 1) + (nsp - 1))

    def row_copy(way, t, c, to):
        cols = pl.ds(c * chunk, chunk)
        return remote(
            raw.at[t, :, cols], raw.at[t, :, cols], rsend.at[way, t // 2], rrecv.at[t, c], sp, to
        )

    def up(t, c):
        return row_copy(0, t, c, lax.rem(tp + 2, ntp))

    def down(t, c):
        return row_copy(1, t, c, lax.rem(tp + ntp - 2, ntp))

    def across(t, c):
        return row_copy(2, t, c, xpeer)

    def forward(t, c, from_below):
        if from_below is not False:

            @pl.when(zi < zn - 1)
            def _():
                up(t, c).start()

        if from_below is not True:

            @pl.when(zi > 0)
            def _():
                down(t, c).start()

        across(t, c).start()

    for c in range(NCH):
        forward(tp, c, None)

    def row_step(s):
        for c in range(NCH):

            @pl.when(zi - s >= 0)
            def _():
                t = tp - 2 * s
                across(t, c).wait_recv()
                forward(t, c, True)

            @pl.when(zi + s < zn)
            def _():
                t = tp + 2 * s
                across(t, c).wait_recv()
                forward(t, c, False)

    copies[1].wait()
    cl = jax.nn.silu(condl[...]).reshape(1, -1)
    cc = jax.nn.silu(condc[...]).reshape(1, -1)
    row = lax.broadcasted_iota(jnp.int32, (8, cl.shape[1]), 0)
    cond = jnp.where(row == 0, cl, jnp.where(row == 1, cc, 0.0)).astype(BF16)
    part[sp] = jnp.dot(cond, modwv[...], preferred_element_type=F32)[0:2]
    def p1(d, src):
        return remote(part.at[src], part.at[src], p1s.at[d], p1r.at[src], lax.rem(sp + d, nsp), tp)

    @pl.loop(1, nsp)
    def _(d):
        p1(d, sp).start()

    @pl.loop(1, nsp)
    def _(d):
        p1(d, lax.rem(sp + nsp - d, nsp)).wait_recv()

    total = part[0]
    for k in range(1, nsp):
        total = total + part[k]
    mods[tp] = total

    def p2(d, src):
        return remote(mods.at[src], mods.at[src], p2s.at[d], p2r.at[src], sp, lax.rem(tp + d, ntp))

    @pl.loop(1, ntp)
    def _(d):
        p2(d, tp).start()

    row_step(1)
    if zn > 2:
        row_step(2)

    mine = pl.ds(pl.multiple_of(ci * hw, hw), hw)

    def wo_copy(i, src, dst, to_sp, to_tp, core):
        return remote(wo.at[src, mine], wo.at[dst, mine], ws.at[i], wr.at[dst, core], to_sp, to_tp)

    wo_z = wo_copy(0, 0, 1, sp, zpeer, ci)
    wo_x = wo_copy(1, 0, 2, sp, xpeer, ci)
    wo_xz = wo_copy(2, 1, 3, sp, xpeer, ci)
    wo_core = [wo_copy(2 + r, r, r, cpeer, tp, ci) for r in range(1, 4)]

    def wo_arrival(r):
        other = pl.ds(pl.multiple_of((1 - ci) * hw, hw), hw)
        return remote(wo.at[r, other], wo.at[r, other], ws.at[2 + r], wr.at[r, 1 - ci], cpeer, tp)

    copies[7].wait()
    wo_z.start()

    @pl.loop(1, ntp)
    def _(d):
        p2(d, lax.rem(tp + ntp - d, ntp)).wait_recv()

    mod = jnp.concatenate([mods[t] for t in range(ntp)], axis=1)
    shift_l, shift_c = mod[0:1, :width], mod[1:2, :width]
    scale_l, scale_c = 1.0 + mod[0:1, width : 2 * width], 1.0 + mod[1:2, width : 2 * width]
    gate = mod[0:1, 2 * width :]

    def normed(x, scale, shift):
        x = x.astype(F32)
        x = x * lax.rsqrt(jnp.mean(x * x, axis=-1, keepdims=True) + NORM_EPS)
        return (x * scale + shift).astype(BF16)

    copies[2].wait()
    nctx[...] = normed(ctxv[...], scale_c, shift_c)
    copies[3].wait()
    copies[4].wait()
    pieces = (pl.ds(0, half), pl.ds(half, half), pl.ds(latrows, ctx))
    kv[sp, latrows:block_rows, :] = jnp.dot(
        nctx[...], wcat[:, 0:256], preferred_element_type=F32
    ).astype(BF16)

    def kv_direct(which, d, src):
        piece = pieces[which]
        return remote(
            kv.at[src, piece], kv.at[src, piece], kvs.at[which, d], kvr.at[which, src],
            lax.rem(sp + 2 * d, nsp), tp,
        )

    def kv_forward(which, src):
        piece = pieces[which]
        return remote(
            kv.at[src, piece], kv.at[src, piece], kvf.at[which, src], kvr.at[which, src], cpeer, tp
        )

    def kv_send(which):
        for d in range(1, yn):
            kv_direct(which, d, sp).start()
        kv_forward(which, sp).start()

    def kv_relay(which):
        for d in range(1, yn):
            src = lax.rem(sp + nsp - 2 * d, nsp)
            kv_direct(which, d, src).wait_recv()
            kv_forward(which, src).start()

    def kv_finish(which):
        for y in range(yn):
            kv_forward(which, y * 2 + (1 - ci)).wait_recv()

    kv_send(2)
    for s in range(3, zn):
        row_step(s)
    wo_x.start()

    nbuf[...] = jnp.zeros_like(nbuf)

    quarter = QK_DIM // 4
    lane = lax.broadcasted_iota(jnp.int32, (1, 128), 1)
    low = lax.rem(lane, 2 * quarter) < quarter

    def rotate(u, k):
        turned = jnp.where(low, pltpu.roll(u, 128 - quarter, 1), pltpu.roll(u, quarter, 1))
        return (u * tab[k, :, 0:128] + turned * tab[k, :, 128:256]).astype(BF16)

    def project(k):
        x = nbuf[k * zn : (k + 1) * zn].reshape(half, width)
        pkv = jnp.dot(x, wcat[:, 0:256], preferred_element_type=F32)
        here = slice(k * half, (k + 1) * half)
        kv[sp, here, 0:128] = rotate(pkv[:, 0:128], k)
        kv[sp, here, 128:256] = pkv[:, 128:256].astype(BF16)
        kv_send(k)
        q = jnp.dot(x, wcat[:, 256:384], preferred_element_type=F32)
        q = rotate(q, k) * BF16(QK_DIM**-0.5)
        for i in range(zn):
            u = q[i * padded : (i + 1) * padded]
            d = lax.rem(i % nq + nq - ki, nq)
            to = pl.ds(pl.multiple_of((d * 4 + k * 2 + i // nq) * padded, padded), padded)
            qbuf[0, to, :] = jnp.where(lane < QK_DIM, u, BF16(0))
            qbuf[1, to, :] = jnp.where(lane < QK_DIM, BF16(0), u)

    def position(i):
        return 2 * (i % nq) + (pz if i < nq else 1 - pz)

    for i in range(zn):
        nbuf[i, 0:rows, :] = normed(raw[position(i) * 2 + xi], scale_l, shift_l)
    copies[5].wait()
    copies[6].wait()
    for i in range(8, 11):
        copies[i].wait()
    project(0)
    kv_relay(2)
    for i in range(zn):
        t = position(i) * 2 + (1 - xi)
        for c in range(NCH):
            across(t, c).wait_recv()
        nbuf[zn + i, 0:rows, :] = normed(raw[t], scale_l, shift_l)
    kv_relay(0)
    project(1)
    wo_z.wait_recv()
    wo_xz.start()
    wo_core[0].start()
    kv_relay(1)
    kv_finish(2)
    kv_finish(0)
    kv_finish(1)

    keys = nsp * block_rows
    col = lax.rem(lax.broadcasted_iota(jnp.int32, (1, keys), 1), block_rows)
    empty = jnp.logical_and(col < latrows, lax.rem(col, padded) >= rows)
    bias = jnp.where(empty, F32(-1e30), F32(0.0))
    factor = lam[0]

    def attend(i):
        here = pl.ds(pl.multiple_of(i * qb, qb), qb)
        mixed = []
        for m in range(2):
            s = lax.dot_general(
                qbuf[m, here, :], kv[:, :, 0:128].reshape(keys, 128), (((1,), (1,)), ((), ())),
                preferred_element_type=F32,
            ) + bias
            w = jnp.exp(s - jnp.max(s, axis=-1, keepdims=True))
            t = jnp.sum(w, axis=-1, keepdims=True)
            o = jnp.dot(
                w.astype(BF16), kv[:, :, 128:256].reshape(keys, 128), preferred_element_type=F32
            )
            mixed.append(o / t)
        h = mixed[0] - factor * mixed[1]
        h = h * lax.rsqrt(jnp.mean(h * h, axis=-1, keepdims=True) + HEAD_EPS)
        att[here, :] = h.astype(BF16)

    group = 4 * padded

    def at_copy(d, r, to):
        return remote(
            att.at[pl.ds(d * group + r * padded, padded)], attx.at[d, :, pl.ds(r * 128, 128)],
            ats.at[d, r], atr.at[d, r], sp, to,
        )

    def attended(d):
        pl.loop(d * (group // qb), (d + 1) * (group // qb))(attend)
        attx[d, :, 0:128] = att[d * group : d * group + padded, :]
        for r, to in ((3, xzpeer), (2, xpeer), (1, zpeer)):
            at_copy(d, r, to).start()

    for d in range(nq - 1, -1, -1):
        attended(d)
    wo_x.wait_recv()
    wo_core[1].start()
    wo_xz.wait_recv()
    wo_core[2].start()
    for r in range(1, 4):
        wo_arrival(r).wait_recv()
    w_all = wo[...].reshape(4 * wo.shape[1], width)

    def out_copy(d, src):
        to = (2 * lax.rem(ki + d, nq) + pz) * 2 + xi
        return remote(send.at[d], outb.at[src], os.at[d], orr.at[src], sp, to)

    for d in range(nq - 1, -1, -1):
        for r in range(1, 4):
            at_copy(d, r, xpeer).wait_recv()
        branch = jnp.dot(attx[d], w_all, preferred_element_type=F32)
        if d:
            send[d] = branch.astype(BF16)
            out_copy(d, ki).start()
    for d in range(1, nq):
        src = lax.rem(ki + nq - d, nq)
        out_copy(d, src).wait_recv()
        branch = branch + outb[src].astype(F32)
    branch = branch * lax.rsqrt(jnp.mean(branch * branch, axis=-1, keepdims=True) + NORM_EPS)
    out[...] = (raw[tp].astype(F32) + gate * branch[:rows]).astype(BF16)

    @pl.loop(1, nsp)
    def _(d):
        p1(d, sp).wait_send()

    @pl.loop(1, ntp)
    def _(d):
        p2(d, tp).wait_send()

    for z in range(zn):

        def sent(way):
            whole = raw.at[z * 2 + xi]
            remote(whole, whole, rsend.at[way, z], rrecv.at[0, 0], sp, xpeer).wait_send()

        @pl.when(jnp.logical_and(z <= zi, zi < zn - 1))
        def _():
            sent(0)

        @pl.when(jnp.logical_and(z >= zi, zi > 0))
        def _():
            sent(1)

        sent(2)
    for which in range(3):
        for d in range(1, yn):
            kv_direct(which, d, sp).wait_send()
        for y in range(yn):
            kv_forward(which, y * 2 + ci).wait_send()
    for c in [wo_z, wo_x, wo_xz] + wo_core:
        c.wait_send()
    for d in range(nq):
        for r in range(1, 4):
            at_copy(d, r, xpeer).wait_send()
    for d in range(1, nq):
        out_copy(d, ki).wait_send()


def shards(nsp, ntp, latent, context, condl, condc, modw, wq, wk, wv, wout, lam):
    rows, width = latent.shape
    ctx = context.shape[0]
    padded = -(-rows // 16) * 16
    latrows = ntp * padded
    block_rows = latrows + ctx
    modcols = modw.shape[1]
    zn = ntp // 2
    qb = 4 * padded
    while qb % 32 == 0 and qb * nsp * block_rows * 4 > 1_000_000:
        qb //= 2
    table = jnp.asarray(rotary_tables(nsp, ntp, rows, padded))
    anyspace = pl.BlockSpec(memory_space=pl.ANY)
    vmem = pl.BlockSpec(memory_space=pltpu.VMEM)
    smem = pl.BlockSpec(memory_space=pltpu.SMEM)
    dma = pltpu.SemaphoreType.DMA
    return pl.pallas_call(
        functools.partial(kernel, nsp, ntp, rows, padded, ctx, width, modcols, qb),
        out_shape=jax.ShapeDtypeStruct((rows, width), BF16),
        in_specs=[anyspace, anyspace, vmem, vmem] + [anyspace] * 5 + [smem, anyspace],
        out_specs=vmem,
        scratch_shapes=[
            pltpu.VMEM((ntp, rows, width), BF16),
            pltpu.VMEM((ctx, width), BF16),
            pltpu.VMEM(modw.shape, BF16),
            pltpu.VMEM((width, 384), BF16),
            pltpu.VMEM((4,) + wout.shape, BF16),
            pltpu.VMEM((2, latrows // 2, 256), F32),
            pltpu.VMEM((nsp, 2, modcols), F32),
            pltpu.VMEM((ntp, 2, modcols), F32),
            pltpu.VMEM((ntp, padded, width), BF16),
            pltpu.VMEM((ctx, width), BF16),
            pltpu.VMEM((nsp, block_rows, 256), BF16),
            pltpu.VMEM((2, latrows, 128), BF16),
            pltpu.VMEM((latrows, 128), BF16),
            pltpu.VMEM((zn // 2, padded, 512), BF16),
            pltpu.VMEM((zn // 2, padded, width), BF16),
            pltpu.VMEM((zn // 2, padded, width), BF16),
            dma((11,)), dma((3, ntp // 2)), dma((ntp, NCH)), dma((nsp,)), dma((nsp,)), dma((ntp,)),
            dma((ntp,)), dma((3, nsp)), dma((3, nsp)), dma((3, nsp)), dma((6,)), dma((4, 2)), dma((zn // 2, 4)),
            dma((zn // 2, 4)),
            dma((zn // 2,)), dma((zn // 2,)),
        ],
        compiler_params=pltpu.CompilerParams(
            collective_id=0, has_side_effects=True, vmem_limit_bytes=60 * 1024 * 1024
        ),
    )(latent, context, condl, condc, modw, wq, wk, wv, wout, lam, table)


def solution(mesh):
    nsp, ntp = mesh.shape["sp"], mesh.shape["tp"]
    placed = (
        P(("sp", "tp"), None),
        P("sp", None),
        P("sp"),
        P("sp"),
        P("sp", "tp"),
        P(None, "tp"),
        P(None, "tp"),
        P(None, "tp"),
        P("tp", None),
        P("tp"),
    )
    return jax.shard_map(
        functools.partial(shards, nsp, ntp), mesh=mesh, in_specs=placed,
        out_specs=P(("sp", "tp"), None), check_vma=False,
    )
```
